32 devices in a mesh: fs: 8 (over z, y), tp: 4 (over x, core).
Axes of the slice: x: 2, y: 2, z: 4, core: 2. Of those that a mesh axis runs over, the one named last changes fastest.
Arguments:
- tokens: bfloat16 [12288, 2048], P('fs', 'tp'), may hold values from -6 to 6
- norm_gain: float32 [2048], P('fs'), may hold values from 0.1 to 1.9
- up_weight: float32 [2048, 8192], P('fs', 'tp'), may hold values from -0.125 to 0.125
- down_weight: float32 [2048, 8192], P('fs', 'tp'), may hold values from -0.0625 to 0.0625
Outputs:
- up_matrix: bfloat16 [2048, 8192], P(None, 'tp')
- down_matrix: bfloat16 [2048, 8192], P(None, 'tp')
- mixed: bfloat16 [12288, 2048], P('fs', 'tp')
The draws below stay inside these ranges and needn't reach their ends.
All inputs are finite; a program needn't handle non-finite values.
Results may differ from the reference program's by a relative error of at most 0.0095.
Values may be sent and summed in bfloat16 or wider, within the bound.
A program may use at most 128 MiB of HBM per device.

```python
import jax
import jax.numpy as jnp
from jax import lax

D = 2048
FF = 8192
TOKENS = 12288
N_TP = 4


def levels(rng, shape, pieces, smallest, high):
    factor_of, own = 1.0, jax.random.fold_in(rng, 6)
    for dim, parts in pieces:
        draws = jnp.exp(jax.random.uniform(jax.random.fold_in(own, dim), (parts,), jnp.float32, smallest / len(pieces), high / len(pieces)))
        factor_of = factor_of * jnp.repeat(draws, shape[dim] // parts).reshape([-1 if axis == dim else 1 for axis in range(len(shape))])
    return factor_of


def bell_draw(stream_key, dims, deviation, most, pieces=(), kind=jnp.bfloat16):
    loudness = levels(stream_key, dims, pieces, -0.22, 0.18) if pieces else 1.0
    drawn = jax.random.normal(stream_key, dims, jnp.float32) * deviation * loudness
    return jnp.minimum(jnp.maximum(drawn, -most), most).astype(kind)


def setup_inputs(seed: int = 0) -> dict:
    arg_keys = jax.random.split(jax.random.key(seed), 5)
    tokens = bell_draw(arg_keys[0], (TOKENS, D), 1.0, 6.0, ((0, 8), (1, 4)))
    norm_gain = jnp.clip(1.0 + 0.18 * jax.random.normal(arg_keys[1], (D,), jnp.float32), 0.1, 1.9)
    up_weight = bell_draw(arg_keys[2], (D, FF), D ** -0.5, 0.125, ((0, 8), (1, 4)), jnp.float32)
    down_weight = bell_draw(arg_keys[3], (D, FF), FF ** -0.5, 0.0625, ((0, 8), (1, 4)), jnp.float32)
    return dict(tokens=tokens, norm_gain=norm_gain, up_weight=up_weight, down_weight=down_weight)


epsilon = 1e-06

def reference(tokens, norm_gain, up_weight, down_weight):
    up_matrix = (norm_gain[:, None] * up_weight).astype(jnp.bfloat16)
    down_matrix = down_weight.astype(jnp.bfloat16)
    widened = tokens.astype(jnp.float32)
    normed = (widened * lax.rsqrt(lax.optimization_barrier(jnp.mean(widened * widened, axis=-1, keepdims=True)) + epsilon)).astype(jnp.bfloat16)
    width = FF // N_TP
    mixed_sum = jnp.zeros((tokens.shape[0], tokens.shape[1]), jnp.float32)
    for group_index in range(N_TP):
        up_block = up_matrix[:, group_index * width:(group_index + 1) * width]
        down_block = down_matrix[:, group_index * width:(group_index + 1) * width]
        up_values = jnp.dot(normed, up_block, preferred_element_type=jnp.float32)
        hidden = jnp.square(jax.nn.relu(up_values)).astype(jnp.bfloat16)
        partial_value = lax.dot_general(hidden, down_block, (((1,), (1,)), ((), ())), preferred_element_type=jnp.float32)
        mixed_sum = mixed_sum + partial_value.astype(jnp.bfloat16).astype(jnp.float32)
    return (up_matrix, down_matrix, mixed_sum.astype(jnp.bfloat16))
```

```python
import functools

import jax
import jax.numpy as jnp
from jax import lax
from jax.experimental import pallas as pl
from jax.experimental.pallas import tpu as pltpu
from jax.sharding import PartitionSpec as P

epsilon = 1e-06
MESH = pl.DeviceIdType.MESH
UP, DOWN, SIDE = 0, 1, 2


def chunks_of(rows, m):
    extra = max(16, rows * (2 + m) // 16 // 16 * 16)
    main, half = rows - extra, rows // 2
    if half % 128 == 0:
        return [(0, half), (half, main - half), (main, extra)]
    return [(0, main), (main, extra)]


def kernel(n, tp, tok_in, gain, up_weight, down_weight, up, down, total,
           stage, tok, hidden, part, pair, cross,
           send_sem, recv_sem, tok_send, tok_recv, pair_send, pair_recv, cross_send, cross_recv, local_sem):
    rows, units = up_weight.shape
    tokens, width = tok_in.shape
    chain = n // 2
    groups = tp // 2
    per_owner = n // tp
    chunks = [chunks_of(rows, 0), chunks_of(rows, 1)]
    extra = len(chunks[0]) - 1
    mains = range(extra)
    halves = extra
    half_rows = rows // halves
    fs, me = lax.axis_index("fs"), lax.axis_index("tp")
    z, y = fs // 2, fs % 2
    group, core = me // 2, me % 2
    partner = group * 2 + 1 - core
    bufs = (up, down)

    def target(way):
        if way == UP:
            return {"fs": jnp.minimum(z + 1, chain - 1) * 2 + y}
        if way == DOWN:
            return {"fs": jnp.maximum(z - 1, 0) * 2 + y}
        return {"fs": z * 2 + 1 - y}

    def spot(m, src, k):
        return pl.ds(pl.multiple_of(pl.multiple_of(src * rows, 16) + chunks[m][k][0], 16), chunks[m][k][1])

    def copy(m, src, k, way):
        where = spot(m, src, k)
        return pltpu.make_async_remote_copy(
            src_ref=bufs[m].at[where],
            dst_ref=bufs[m].at[where],
            send_sem=send_sem.at[m, way],
            recv_sem=recv_sem.at[m, src, k],
            device_id=target(way),
            device_id_type=MESH,
        )

    def arrived(m, src, k):
        where = spot(m, src, k)
        pltpu.make_async_remote_copy(
            src_ref=bufs[m].at[where], dst_ref=bufs[m].at[where],
            send_sem=send_sem.at[m, SIDE], recv_sem=recv_sem.at[m, src, k],
            device_id=target(SIDE), device_id_type=MESH,
        ).wait_recv()

    along = [(way, k) for k in mains for way in (UP, DOWN)]
    beside = [(SIDE, extra)] + [(SIDE, k) for k in mains]

    def when_way(way, fn):
        if way == UP:
            pl.when(z < chain - 1)(fn)
        elif way == DOWN:
            pl.when(z > 0)(fn)
        else:
            fn()

    def start_own(m, order):
        for way, k in order:
            when_way(way, lambda way=way, k=k: copy(m, fs, k, way).start())

    middle = (z > 0) & (z < chain - 1)
    opposite = z * 2 + 1 - y

    def own_extras(m, late):
        for way in (UP, DOWN):
            edge = middle & (z == (chain - 2 if way == UP else 1))
            now = edge if late else jnp.logical_not(edge)

            def send(way=way):
                copy(m, fs, extra, way).start()
                copy(m, opposite, extra, way).start()

            when_way(way, lambda now=now, send=send: pl.when(now)(send))

    def step_sends(m, d, act, wait, plan):
        for k, flip in plan:
            for sign, way in ((-1, UP), (1, DOWN)):
                at = z + sign * d
                src = at * 2 + (y + flip) % 2

                @pl.when((at >= 0) & (at < chain))
                def _():
                    if wait:
                        arrived(m, src, k)
                    when_way(way, lambda: act(copy(m, src, k, way)))
                    if k != extra:
                        act(copy(m, src, k, SIDE))

    def side_arrivals(m, d):
        for sign in (-1, 1) if not (isinstance(d, int) and d == 0) else (1,):
            at = z + sign * d

            @pl.when((at >= 0) & (at < chain))
            def _():
                for k in mains:
                    arrived(m, at * 2 + 1 - y, k)

    main_plan = [(k, 0) for k in mains]
    extra_plan = [(extra, 0), (extra, 1)]

    def forward(m, d, plan):
        step_sends(m, d, lambda c: c.start(), True, plan)

    own_rows = pl.ds(pl.multiple_of(fs * rows, 16), rows)
    loads = [pltpu.make_async_copy(up_weight, stage.at[0], local_sem.at[1]),
             pltpu.make_async_copy(tok_in, tok.at[:, pl.ds(pl.multiple_of(me * width, 128), width)], local_sem.at[0]),
             pltpu.make_async_copy(down_weight, stage.at[1], local_sem.at[2])]
    for load in loads:
        load.start()

    barrier = pltpu.get_barrier_semaphore()
    greet = [target(SIDE), {"tp": partner}]
    greet += [{"tp": lax.rem(group + g, groups) * 2 + core} for g in range(1, groups)]

    def hello(who):
        pl.semaphore_signal(barrier, inc=1, device_id=who, device_id_type=MESH)

    for way in (UP, DOWN):
        when_way(way, lambda way=way: hello(target(way)))
    for who in greet:
        hello(who)
    callers = len(greet) + (z > 0).astype(jnp.int32) + (z < chain - 1).astype(jnp.int32)
    loads[0].wait()
    by_row = jnp.transpose(jnp.broadcast_to(gain[...], (128, rows)))[:, :1]
    up[own_rows, :] = (by_row * stage[0]).astype(jnp.bfloat16)
    pl.semaphore_wait(barrier, callers)

    start_own(0, [(way, k) for k in mains for way in (UP, DOWN, SIDE)] + [(SIDE, extra)])
    loads[1].wait()

    def columns(owner):
        return pl.ds(pl.multiple_of(owner * width, 128), width)

    def token_copy(owner, to, slot):
        return pltpu.make_async_remote_copy(
            src_ref=tok.at[:, columns(owner)],
            dst_ref=tok.at[:, columns(owner)],
            send_sem=tok_send.at[slot], recv_sem=tok_recv.at[owner],
            device_id={"tp": to}, device_id_type=MESH)

    across = [lax.rem(group + g, groups) * 2 + core for g in range(1, groups)]
    back = [lax.rem(group + groups - g, groups) * 2 + core for g in range(1, groups)]
    token_sends = [token_copy(me, to, i) for i, to in enumerate(across)]
    token_sends.append(token_copy(me, partner, groups - 1))
    for c in token_sends:
        c.start()
    loads[2].wait()
    down[own_rows, :] = stage[1].astype(jnp.bfloat16)

    forward(0, 1, main_plan)
    arrived(0, opposite, extra)
    own_extras(0, False)
    own_extras(0, True)
    pl.when(jnp.logical_not(middle))(lambda: start_own(1, along))

    relays = []
    for i, owner in enumerate(back):
        token_copy(owner, partner, groups + i).wait_recv()
        c = token_copy(owner, partner, groups + i)
        c.start()
        relays.append(c)
    forward(0, 2, main_plan)
    token_copy(partner, partner, 0).wait_recv()
    for g in range(1, groups):
        token_copy(lax.rem(group + g, groups) * 2 + 1 - core, partner, 0).wait_recv()
    for c in token_sends + relays:
        c.wait_send()
    tile = 128

    @pl.loop(0, tokens // tile)
    def _(i):
        at = pl.ds(pl.multiple_of(i * tile, tile), tile)
        wide = tok[at, :].astype(jnp.float32)
        scale = lax.rsqrt(jnp.mean(wide * wide, axis=-1, keepdims=True) + epsilon)
        tok[at, :] = (wide * scale).astype(jnp.bfloat16)

    for d in range(3, chain):
        forward(0, d, main_plan)
    start_own(1, beside)
    for d in range(1, chain):
        forward(0, d, extra_plan)
    pl.when(middle)(lambda: start_own(1, along))
    for d in range(chain):
        side_arrivals(0, d)
    bm, bn = min(512, tokens), min(512, units)

    def expand(first, last):
        @pl.loop(first, last)
        def _(j):
            cols = pl.ds(pl.multiple_of(j * bn, bn), bn)

            @pl.loop(0, tokens // bm)
            def _(i):
                at = pl.ds(pl.multiple_of(i * bm, bm), bm)
                values = jnp.dot(tok[at, :], up[:, cols], preferred_element_type=jnp.float32)
                values = jnp.maximum(values, 0.0)
                hidden[at, cols] = (values * values).astype(jnp.bfloat16)

    parts = units // bn
    expand(0, parts // 2)
    arrived(1, opposite, extra)
    own_extras(1, False)
    forward(1, 1, main_plan[:1])
    expand(parts // 2, parts * 3 // 4)
    forward(1, 1, main_plan[1:])
    expand(parts * 3 // 4, parts)

    def pair_copy(r, h):
        return pltpu.make_async_remote_copy(
            src_ref=part.at[r, h], dst_ref=pair.at[r, h], send_sem=pair_send.at[0], recv_sem=pair_recv.at[r, h],
            device_id={"tp": partner}, device_id_type=MESH)

    def cross_copy(r, h, to_group, from_group):
        slot = r % per_owner
        return pltpu.make_async_remote_copy(
            src_ref=part.at[r, h], dst_ref=cross.at[from_group, slot, h],
            send_sem=cross_send.at[0], recv_sem=cross_recv.at[from_group, slot, h],
            device_id={"tp": to_group * 2 + core}, device_id_type=MESH)

    def multiply(r, hs):
        where = pl.ds(pl.multiple_of(r * rows + hs[0] * half_rows, 16), len(hs) * half_rows)

        @pl.loop(0, tokens // bm)
        def _(i):
            at = pl.ds(pl.multiple_of(i * bm, bm), bm)
            values = lax.dot_general(
                hidden[at, :], down[where, :], (((1,), (1,)), ((), ())),
                preferred_element_type=jnp.float32).astype(jnp.bfloat16)
            for i_h, h in enumerate(hs):
                part[r, h, at, :] = values[:, i_h * half_rows:(i_h + 1) * half_rows]

        @pl.when(r // per_owner % 2 != core)
        def _():
            for h in hs:
                pair_copy(r, h).start()

    def pair_sum(r, hs):
        owner = r // per_owner

        @pl.when(owner % 2 == core)
        def _():
            for h in hs:
                pair_copy(r, h).wait_recv()

                @pl.loop(0, tokens // tile)
                def _(i):
                    at = pl.ds(pl.multiple_of(i * tile, tile), tile)
                    both = part[r, h, at, :].astype(jnp.float32) + pair[r, h, at, :].astype(jnp.float32)
                    part[r, h, at, :] = both.astype(jnp.bfloat16)

                @pl.when(owner // 2 != group)
                def _():
                    cross_copy(r, h, owner // 2, group).start()

    def at_distance(d, flip, fn):
        for sign in (-1, 1):
            at = z + sign * d

            @pl.when((at >= 0) & (at < chain))
            def _():
                fn(at * 2 + (y + flip) % 2)

    every = list(range(halves))

    first, rest = every[:1], every[1:]
    last = chain - 1
    head, tail = (first, rest) if rest else ([], every)

    def opposite_block(h):
        arrived(1, opposite, h)
        multiply(opposite, [h])

    def near_flow():
        def side(d, hs):
            def run(r):
                for h in hs:
                    arrived(1, r, h)
                    multiply(r, [h])

            at_distance(d, 1, run)

        def sums(d, flip, hs):
            at_distance(d, flip, lambda r: pair_sum(r, hs))

        if head:
            at_distance(1, 0, lambda r: multiply(r, head))

        @pl.loop(2, last)
        def _(d):
            forward(1, d, main_plan)

        @pl.loop(1, last)
        def _(d):
            forward(1, d, extra_plan)

        own_extras(1, True)
        pair_sum(opposite, first)
        sums(1, 0, head)
        for h in rest:
            opposite_block(h)
        at_distance(1, 0, lambda r: multiply(r, tail))
        pair_sum(opposite, rest)

        @pl.loop(2, last)
        def _(d):
            at_distance(d, 0, lambda r: multiply(r, every))

        sums(1, 0, tail)
        side(1, first)

        @pl.loop(2, last)
        def _(d):
            sums(d, 0, every)

        sums(1, 1, first)
        side(1, rest)
        sums(1, 1, rest)

        @pl.loop(2, last)
        def _(d):
            side(d, first)
            sums(d, 1, first)
            side(d, rest)
            sums(d, 1, rest)

    def end_flow():
        def far(d, flip):
            return jnp.where(z == 0, d, last - d) * 2 + (y + flip) % 2

        def take(d, k, flip=0):
            r = far(d, flip)
            arrived(1, r, k)
            if k != extra:
                copy(1, r, k, SIDE).start()

        def main(d, hs):
            if hs:
                multiply(far(d, 0), hs)

        def side(d, hs):
            for h in hs:
                arrived(1, far(d, 1), h)
                multiply(far(d, 1), [h])

        def sums(d, flip, hs):
            pair_sum(far(d, flip), hs)

        main(1, head)
        pair_sum(opposite, first)
        for h in rest:
            opposite_block(h)
        sums(1, 0, head)
        pair_sum(opposite, rest)

        @pl.loop(2, chain)
        def _(d):
            take(d, 0)
            main(d, head)
            side(d - 1, head)
            sums(d, 0, head)
            for k in mains[1:]:
                take(d, k)
            sums(d - 1, 1, head)

        @pl.loop(2, last)
        def _(d):
            take(d, extra)
            main(d, tail)
            take(d, extra, 1)
            sums(d, 0, tail)
            side(d, tail)
            sums(d, 1, tail)

        take(last, extra)
        main(last, tail)
        take(last, extra, 1)
        sums(last, 0, tail)
        side(last, head)
        take(1, extra)
        main(1, tail)
        sums(last, 1, head)
        take(1, extra, 1)
        sums(1, 0, tail)
        side(1, tail)
        side(last, tail)
        sums(1, 1, tail)
        sums(last, 1, tail)

    multiply(fs, every)
    opposite_block(0)
    pair_sum(fs, every)
    pl.when(middle)(near_flow)
    pl.when(jnp.logical_not(middle))(end_flow)

    for s in range(per_owner):
        r = me * per_owner + s
        for h in every:
            for g in range(1, groups):
                other = lax.rem(group + g, groups)
                cross_copy(r, h, other, other).wait_recv()

            @pl.loop(0, tokens // tile)
            def _(i):
                at = pl.ds(pl.multiple_of(i * tile, tile), tile)
                value = part[r, h, at, :].astype(jnp.float32)
                for g in range(1, groups):
                    value = value + cross[lax.rem(group + g, groups), s, h, at, :].astype(jnp.float32)
                first = s * rows + h * half_rows
                total[at, first:first + half_rows] = value.astype(jnp.bfloat16)

    for m in (0, 1):
        spread = rows + chunks[m][extra][1]

        def sent(way, count):
            where = pl.ds(0, count)
            pltpu.make_async_remote_copy(
                src_ref=bufs[m].at[where], dst_ref=bufs[m].at[where],
                send_sem=send_sem.at[m, way], recv_sem=recv_sem.at[m, fs, 0],
                device_id=target(way), device_id_type=MESH).wait_send()

        sent(SIDE, rows + (chain - 1) * (rows - chunks[m][extra][1]))
        for i in range(last):
            pl.when(z == i)(lambda i=i: sent(UP, (i + 1) * spread))
            pl.when(z == last - i)(lambda i=i: sent(DOWN, (i + 1) * spread))

    def all_sent(sem, recv, count, who):
        where = pl.ds(0, count)
        pltpu.make_async_remote_copy(
            src_ref=part.at[where], dst_ref=part.at[where], send_sem=sem, recv_sem=recv,
            device_id={"tp": who}, device_id_type=MESH).wait_send()

    all_sent(pair_send.at[0], pair_recv.at[0, 0], n // 2, partner)
    if groups > 1:
        all_sent(cross_send.at[0], cross_recv.at[0, 0, 0], per_owner * (groups - 1), partner)


pieces = 4


def store(up, down, total, up_out, down_out, total_out, sem):
    copies = []
    for i, (src, dst) in enumerate(((up, up_out), (down, down_out), (total, total_out))):
        step = src.shape[0] // pieces
        for j in range(pieces):
            at = pl.ds(j * step, step)
            copies.append(pltpu.make_async_copy(src.at[at], dst.at[at], sem.at[i, j]))
    for c in copies:
        c.start()
    for c in copies:
        c.wait()


def on_device(n, tp, tokens, norm_gain, up_weight, down_weight):
    rows, units = up_weight.shape
    count, width = tokens.shape
    bf16 = jnp.bfloat16
    groups, per_owner = tp // 2, n // tp
    chunks = len(chunks_of(rows, 0))
    halves = chunks - 1
    half_rows = rows // halves
    features = width * tp
    dma = pltpu.SemaphoreType.DMA
    flops = 2 * 2 * count * features * units
    results = pl.pallas_call(
        functools.partial(kernel, n, tp),
        out_shape=(pltpu.VMEM((features, units), bf16), pltpu.VMEM((features, units), bf16),
                   pltpu.VMEM((count, width), bf16)),
        in_specs=[pl.BlockSpec(memory_space=pl.ANY if i != 1 else pltpu.VMEM) for i in range(4)],
        out_specs=[pl.BlockSpec(memory_space=pltpu.VMEM)] * 3,
        scratch_shapes=[
            pltpu.VMEM((2, rows, units), jnp.float32),
            pltpu.VMEM((count, features), bf16),
            pltpu.VMEM((count, units), bf16),
            pltpu.VMEM((n, halves, count, half_rows), bf16),
            pltpu.VMEM((n, halves, count, half_rows), bf16),
            pltpu.VMEM((groups, per_owner, halves, count, half_rows), bf16),
            dma((2, 3)), dma((2, n, chunks)),
            dma((2 * groups,)), dma((tp,)),
            dma((1,)), dma((n, halves)), dma((1,)), dma((groups, per_owner, halves)),
            dma((3,)),
        ],
        cost_estimate=pl.CostEstimate(flops=flops, bytes_accessed=4 * features * units * 2, transcendentals=0),
        compiler_params=pltpu.CompilerParams(
            collective_id=0, has_side_effects=True, vmem_limit_bytes=44 << 20),
    )(tokens, norm_gain[None, :], up_weight, down_weight)
    return tuple(pl.pallas_call(
        store,
        out_shape=[jax.ShapeDtypeStruct(r.shape, r.dtype) for r in results],
        in_specs=[pl.BlockSpec(memory_space=pl.ANY)] * 3,
        out_specs=[pl.BlockSpec(memory_space=pltpu.HBM)] * 3,
        scratch_shapes=[dma((3, pieces))],
        compiler_params=pltpu.CompilerParams(vmem_limit_bytes=1 << 20),
    )(*results))


def solution(mesh):
    return jax.shard_map(
        functools.partial(on_device, mesh.shape["fs"], mesh.shape["tp"]),
        mesh=mesh,
        in_specs=(P("fs", "tp"), P("fs"), P("fs", "tp"), P("fs", "tp")),
        out_specs=(P(None, "tp"), P(None, "tp"), P("fs", "tp")),
        check_vma=False,
    )
```

```python
import functools

import jax
import jax.numpy as jnp
from jax import lax
from jax.experimental import pallas as pl
from jax.experimental.pallas import tpu as pltpu
from jax.sharding import PartitionSpec as P

epsilon = 1e-06
MESH = pl.DeviceIdType.MESH
UP, DOWN, SIDE = 0, 1, 2


def chunks_of(rows, m):
    extra = max(16, rows * (2 + m) // 16 // 16 * 16)
    main, half = rows - extra, rows // 2
    if half % 128 == 0:
        return [(0, half), (half, main - half), (main, extra)]
    return [(0, main), (main, extra)]


def kernel(n, tp, tok_in, gain, up_weight, down_weight, up, down, total,
           stage, tok, hidden, part, pair, cross,
           send_sem, recv_sem, tok_send, tok_recv, pair_send, pair_recv, cross_send, cross_recv, local_sem):
    rows, units = up_weight.shape
    tokens, width = tok_in.shape
    chain = n // 2
    groups = tp // 2
    per_owner = n // tp
    chunks = [chunks_of(rows, 0), chunks_of(rows, 1)]
    extra = len(chunks[0]) - 1
    mains = range(extra)
    halves = extra
    half_rows = rows // halves
    fs, me = lax.axis_index("fs"), lax.axis_index("tp")
    z, y = fs // 2, fs % 2
    group, core = me // 2, me % 2
    partner = group * 2 + 1 - core
    bufs = (up, down)

    def target(way):
        if way == UP:
            return {"fs": jnp.minimum(z + 1, chain - 1) * 2 + y}
        if way == DOWN:
            return {"fs": jnp.maximum(z - 1, 0) * 2 + y}
        return {"fs": z * 2 + 1 - y}

    def spot(m, src, k):
        return pl.ds(pl.multiple_of(pl.multiple_of(src * rows, 16) + chunks[m][k][0], 16), chunks[m][k][1])

    def copy(m, src, k, way):
        where = spot(m, src, k)
        return pltpu.make_async_remote_copy(
            src_ref=bufs[m].at[where],
            dst_ref=bufs[m].at[where],
            send_sem=send_sem.at[m, way],
            recv_sem=recv_sem.at[m, src, k],
            device_id=target(way),
            device_id_type=MESH,
        )

    def arrived(m, src, k):
        where = spot(m, src, k)
        pltpu.make_async_remote_copy(
            src_ref=bufs[m].at[where], dst_ref=bufs[m].at[where],
            send_sem=send_sem.at[m, SIDE], recv_sem=recv_sem.at[m, src, k],
            device_id=target(SIDE), device_id_type=MESH,
        ).wait_recv()

    along = [(way, k) for k in mains for way in (UP, DOWN)]
    beside = [(SIDE, extra)] + [(SIDE, k) for k in mains]

    def when_way(way, fn):
        if way == UP:
            pl.when(z < chain - 1)(fn)
        elif way == DOWN:
            pl.when(z > 0)(fn)
        else:
            fn()

    def start_own(m, order):
        for way, k in order:
            when_way(way, lambda way=way, k=k: copy(m, fs, k, way).start())

    middle = (z > 0) & (z < chain - 1)
    opposite = z * 2 + 1 - y

    def own_extras(m, late):
        for way in (UP, DOWN):
            edge = middle & (z == (chain - 2 if way == UP else 1))
            now = edge if late else jnp.logical_not(edge)

            def send(way=way):
                copy(m, fs, extra, way).start()
                copy(m, opposite, extra, way).start()

            when_way(way, lambda now=now, send=send: pl.when(now)(send))

    def step_sends(m, d, act, wait, plan):
        for k, flip in plan:
            for sign, way in ((-1, UP), (1, DOWN)):
                at = z + sign * d
                src = at * 2 + (y + flip) % 2

                @pl.when((at >= 0) & (at < chain))
                def _():
                    if wait:
                        arrived(m, src, k)
                    when_way(way, lambda: act(copy(m, src, k, way)))
                    if k != extra:
                        act(copy(m, src, k, SIDE))

    def side_arrivals(m, d):
        for sign in (-1, 1) if not (isinstance(d, int) and d == 0) else (1,):
            at = z + sign * d

            @pl.when((at >= 0) & (at < chain))
            def _():
                for k in mains:
                    arrived(m, at * 2 + 1 - y, k)

    main_plan = [(k, 0) for k in mains]
    extra_plan = [(extra, 0), (extra, 1)]

    def forward(m, d, plan):
        step_sends(m, d, lambda c: c.start(), True, plan)

    own_rows = pl.ds(pl.multiple_of(fs * rows, 16), rows)
    lead = chunks[0][0][1]
    lead_rows, other_rows = pl.ds(0, lead), pl.ds(lead, rows - lead)
    loads = [pltpu.make_async_copy(up_weight.at[lead_rows], stage.at[0, lead_rows], local_sem.at[0]),
             pltpu.make_async_copy(up_weight.at[other_rows], stage.at[0, other_rows], local_sem.at[1]),
             pltpu.make_async_copy(tok_in, tok.at[:, pl.ds(pl.multiple_of(me * width, 128), width)], local_sem.at[2]),
             pltpu.make_async_copy(down_weight, stage.at[1], local_sem.at[3])]
    for load in loads[:2]:
        load.start()

    barrier = pltpu.get_barrier_semaphore()
    greet = [target(SIDE), {"tp": partner}]
    greet += [{"tp": lax.rem(group + g, groups) * 2 + core} for g in range(1, groups)]

    def hello(who):
        pl.semaphore_signal(barrier, inc=1, device_id=who, device_id_type=MESH)

    for way in (UP, DOWN):
        when_way(way, lambda way=way: hello(target(way)))
    for who in greet:
        hello(who)
    callers = len(greet) + (z > 0).astype(jnp.int32) + (z < chain - 1).astype(jnp.int32)
    by_row = jnp.transpose(jnp.broadcast_to(gain[...], (128, rows)))[:, :1]

    def scaled(first, count):
        at = pl.ds(pl.multiple_of(fs * rows + first, 16), count)
        up[at, :] = (by_row[first:first + count] * stage[0, first:first + count]).astype(jnp.bfloat16)

    loads[0].wait()
    for load in loads[2:]:
        load.start()
    scaled(0, lead)
    pl.semaphore_wait(barrier, callers)
    start_own(0, [(way, 0) for way in (UP, DOWN, SIDE)])
    loads[1].wait()
    scaled(lead, rows - lead)
    start_own(0, [(way, k) for k in mains[1:] for way in (UP, DOWN, SIDE)] + [(SIDE, extra)])
    loads[2].wait()

    def columns(owner):
        return pl.ds(pl.multiple_of(owner * width, 128), width)

    def token_copy(owner, to, slot):
        return pltpu.make_async_remote_copy(
            src_ref=tok.at[:, columns(owner)],
            dst_ref=tok.at[:, columns(owner)],
            send_sem=tok_send.at[slot], recv_sem=tok_recv.at[owner],
            device_id={"tp": to}, device_id_type=MESH)

    across = [lax.rem(group + g, groups) * 2 + core for g in range(1, groups)]
    back = [lax.rem(group + groups - g, groups) * 2 + core for g in range(1, groups)]
    token_sends = [token_copy(me, to, i) for i, to in enumerate(across)]
    token_sends.append(token_copy(me, partner, groups - 1))
    for c in token_sends:
        c.start()
    loads[3].wait()
    down[own_rows, :] = stage[1].astype(jnp.bfloat16)

    forward(0, 1, main_plan)
    arrived(0, opposite, extra)
    own_extras(0, False)
    own_extras(0, True)
    pl.when(jnp.logical_not(middle))(lambda: start_own(1, along))

    relays = []
    for i, owner in enumerate(back):
        token_copy(owner, partner, groups + i).wait_recv()
        c = token_copy(owner, partner, groups + i)
        c.start()
        relays.append(c)
    forward(0, 2, main_plan)
    token_copy(partner, partner, 0).wait_recv()
    for g in range(1, groups):
        token_copy(lax.rem(group + g, groups) * 2 + 1 - core, partner, 0).wait_recv()
    for c in token_sends + relays:
        c.wait_send()
    tile = 128

    @pl.loop(0, tokens // tile)
    def _(i):
        at = pl.ds(pl.multiple_of(i * tile, tile), tile)
        wide = tok[at, :].astype(jnp.float32)
        scale = lax.rsqrt(jnp.mean(wide * wide, axis=-1, keepdims=True) + epsilon)
        tok[at, :] = (wide * scale).astype(jnp.bfloat16)

    for d in range(3, chain):
        forward(0, d, main_plan)
    start_own(1, beside)
    for d in range(1, chain):
        forward(0, d, extra_plan)
    pl.when(middle)(lambda: start_own(1, along))
    for d in range(chain):
        side_arrivals(0, d)
    bm, bn = min(512, tokens), min(512, units)

    def expand(first, last):
        @pl.loop(first, last)
        def _(j):
            cols = pl.ds(pl.multiple_of(j * bn, bn), bn)

            @pl.loop(0, tokens // bm)
            def _(i):
                at = pl.ds(pl.multiple_of(i * bm, bm), bm)
                values = jnp.dot(tok[at, :], up[:, cols], preferred_element_type=jnp.float32)
                values = jnp.maximum(values, 0.0)
                hidden[at, cols] = (values * values).astype(jnp.bfloat16)

    parts = units // bn
    expand(0, parts // 2)
    arrived(1, opposite, extra)
    own_extras(1, False)
    forward(1, 1, main_plan[:1])
    expand(parts // 2, parts * 3 // 4)
    forward(1, 1, main_plan[1:])
    expand(parts * 3 // 4, parts)

    tiles = tokens // bm

    def tile_rows(i):
        return pl.ds(pl.multiple_of(i * bm, bm), bm)

    def pair_copy(r, h, i):
        return pltpu.make_async_remote_copy(
            src_ref=part.at[r, h, tile_rows(i)], dst_ref=pair.at[r, h, tile_rows(i)],
            send_sem=pair_send.at[0], recv_sem=pair_recv.at[r, h, i],
            device_id={"tp": partner}, device_id_type=MESH)

    def cross_copy(r, h, i, to_group, from_group):
        slot = r % per_owner
        return pltpu.make_async_remote_copy(
            src_ref=part.at[r, h, tile_rows(i)], dst_ref=cross.at[from_group, slot, h, tile_rows(i)],
            send_sem=cross_send.at[0], recv_sem=cross_recv.at[from_group, slot, h, i],
            device_id={"tp": to_group * 2 + core}, device_id_type=MESH)

    def multiply(r, hs, after=lambda i: None):
        where = pl.ds(pl.multiple_of(r * rows + hs[0] * half_rows, 16), len(hs) * half_rows)

        @pl.loop(0, tiles)
        def _(i):
            at = tile_rows(i)
            values = lax.dot_general(
                hidden[at, :], down[where, :], (((1,), (1,)), ((), ())),
                preferred_element_type=jnp.float32).astype(jnp.bfloat16)
            for i_h, h in enumerate(hs):
                part[r, h, at, :] = values[:, i_h * half_rows:(i_h + 1) * half_rows]

            @pl.when(r // per_owner % 2 != core)
            def _():
                for h in hs:
                    pair_copy(r, h, i).start()

            after(i)

    def pair_tile(r, hs, i):
        owner = r // per_owner

        @pl.when(owner % 2 == core)
        def _():
            at = tile_rows(i)
            for h in hs:
                pair_copy(r, h, i).wait_recv()
                both = part[r, h, at, :].astype(jnp.float32) + pair[r, h, at, :].astype(jnp.float32)
                part[r, h, at, :] = both.astype(jnp.bfloat16)
                pl.when(owner // 2 != group)(lambda h=h: cross_copy(r, h, i, owner // 2, group).start())

    def pair_sum(r, hs):
        if hs:
            pl.loop(0, tiles)(lambda i: pair_tile(r, hs, i))

    def eager(r, hs):
        return lambda i: pl.when(core == 0)(lambda: pair_tile(r, hs, i))

    def later(r, hs):
        pl.when(core == 1)(lambda: pair_sum(r, hs))

    def at_distance(d, flip, fn):
        for sign in (-1, 1):
            at = z + sign * d

            @pl.when((at >= 0) & (at < chain))
            def _():
                fn(at * 2 + (y + flip) % 2)

    every = list(range(halves))

    first, rest = every[:1], every[1:]
    last = chain - 1
    outer = (z <= 1) | (z >= last - 1)
    final = jnp.where(z <= 1, last, 0) * 2 + 1 - y
    head, tail = (first, rest) if rest else ([], every)

    def opposite_block(h):
        arrived(1, opposite, h)
        multiply(opposite, [h])

    def final_block(meanwhile):
        h = every[-1]

        def after(i):
            pl.when(core == 0)(lambda: pair_tile(final, [h], i))
            pl.when(core == 1)(lambda: meanwhile(i))

        arrived(1, final, h)
        multiply(final, [h], after)

    def near_flow():
        def side(d, hs):
            def run(r):
                for h in hs:
                    arrived(1, r, h)
                    multiply(r, [h])

            at_distance(d, 1, run)

        def sums(d, flip, hs):
            at_distance(d, flip, lambda r: pair_sum(r, hs))

        if head:
            at_distance(1, 0, lambda r: multiply(r, head))

        @pl.loop(2, last)
        def _(d):
            forward(1, d, main_plan)

        @pl.loop(1, last - 1)
        def _(d):
            forward(1, d, extra_plan)

        forward(1, last - 1, extra_plan[:1])
        own_extras(1, True)
        forward(1, last - 1, extra_plan[1:])
        pair_sum(opposite, first)
        sums(1, 0, head)
        for h in rest:
            opposite_block(h)
        at_distance(1, 0, lambda r: multiply(r, tail))
        pair_sum(opposite, rest)

        @pl.loop(2, last)
        def _(d):
            at_distance(d, 0, lambda r: multiply(r, every))

        sums(1, 0, tail)
        side(1, first)

        @pl.loop(2, last)
        def _(d):
            sums(d, 0, every)

        sums(1, 1, first)
        side(1, rest)
        sums(1, 1, rest)

        @pl.loop(2, last - 1)
        def _(d):
            side(d, every)
            sums(d, 1, every)

        @pl.when(outer)
        def _():
            before = every[:-1]
            for h in before:
                arrived(1, final, h)
                multiply(final, [h], eager(final, [h]))
            later(final, before)
            final_block(lambda i: None)
            later(final, every[-1:])

    def end_flow():
        def far(d, flip):
            return jnp.where(z == 0, d, last - d) * 2 + (y + flip) % 2

        def take(d, k, flip=0):
            r = far(d, flip)
            arrived(1, r, k)
            if k != extra:
                copy(1, r, k, SIDE).start()

        def main(d, hs, soon=False):
            r = far(d, 0)
            if hs:
                multiply(r, hs, *([eager(r, hs)] if soon else []))

        def side(d, hs, soon=False):
            r = far(d, 1)
            for h in hs:
                arrived(1, r, h)
                multiply(r, [h], *([eager(r, [h])] if soon else []))

        def sums(d, flip, hs):
            pair_sum(far(d, flip), hs)

        main(1, head)
        pair_sum(opposite, first)
        for h in rest:
            opposite_block(h)
        sums(1, 0, head)
        pair_sum(opposite, rest)

        @pl.loop(2, chain)
        def _(d):
            take(d, 0)
            main(d, head)
            sums(d, 0, head)
            side(d - 1, head)
            for k in mains[1:]:
                take(d, k)
            sums(d - 1, 1, head)

        @pl.loop(2, last)
        def _(d):
            take(d, extra)
            main(d, tail)
            take(d, extra, 1)
            sums(d, 0, tail)
            side(d, tail)
            sums(d, 1, tail)

        take(last, extra)
        main(last, tail, True)
        take(1, extra)
        main(1, tail, True)
        later(far(last, 0), tail)
        side(last, head, True)
        later(far(1, 0), tail)
        take(1, extra, 1)
        side(1, tail, True)
        later(final, head)
        take(last, extra, 1)
        final_block(lambda i: pair_tile(far(1, 1), tail, i))
        later(final, every[-1:])

    multiply(fs, every)
    opposite_block(0)
    pair_sum(fs, every)
    pl.when(middle)(near_flow)
    pl.when(jnp.logical_not(middle))(end_flow)

    for s in range(per_owner):
        r = me * per_owner + s
        for h in every:
            first_column = s * rows + h * half_rows

            @pl.loop(0, tiles)
            def _(i):
                at = tile_rows(i)
                value = part[r, h, at, :].astype(jnp.float32)
                for g in range(1, groups):
                    other = lax.rem(group + g, groups)
                    cross_copy(r, h, i, other, other).wait_recv()
                    value = value + cross[other, s, h, at, :].astype(jnp.float32)
                total[at, first_column:first_column + half_rows] = value.astype(jnp.bfloat16)

    for m in (0, 1):
        spread = rows + chunks[m][extra][1]

        def sent(way, count):
            where = pl.ds(0, count)
            pltpu.make_async_remote_copy(
                src_ref=bufs[m].at[where], dst_ref=bufs[m].at[where],
                send_sem=send_sem.at[m, way], recv_sem=recv_sem.at[m, fs, 0],
                device_id=target(way), device_id_type=MESH).wait_send()

        sent(SIDE, rows + (chain - 1) * (rows - chunks[m][extra][1]))
        for i in range(last):
            pl.when(z == i)(lambda i=i: sent(UP, (i + 1) * spread))
            pl.when(z == last - i)(lambda i=i: sent(DOWN, (i + 1) * spread))

    def all_sent(sem, recv, count, who):
        where = pl.ds(0, count)
        pltpu.make_async_remote_copy(
            src_ref=part.at[where], dst_ref=part.at[where], send_sem=sem, recv_sem=recv,
            device_id={"tp": who}, device_id_type=MESH).wait_send()

    all_sent(pair_send.at[0], pair_recv.at[0, 0, 0], n // 2, partner)
    if groups > 1:
        all_sent(cross_send.at[0], cross_recv.at[0, 0, 0, 0], per_owner * (groups - 1), partner)


pieces = 4


def store(up, down, total, up_out, down_out, total_out, sem):
    copies = []
    for i, (src, dst) in enumerate(((up, up_out), (down, down_out), (total, total_out))):
        step = src.shape[0] // pieces
        for j in range(pieces):
            at = pl.ds(j * step, step)
            copies.append(pltpu.make_async_copy(src.at[at], dst.at[at], sem.at[i, j]))
    for c in copies:
        c.start()
    for c in copies:
        c.wait()


def on_device(n, tp, tokens, norm_gain, up_weight, down_weight):
    rows, units = up_weight.shape
    count, width = tokens.shape
    bf16 = jnp.bfloat16
    groups, per_owner = tp // 2, n // tp
    chunks = len(chunks_of(rows, 0))
    halves = chunks - 1
    half_rows = rows // halves
    features = width * tp
    tiles = count // min(512, count)
    dma = pltpu.SemaphoreType.DMA
    flops = 2 * 2 * count * features * units
    results = pl.pallas_call(
        functools.partial(kernel, n, tp),
        out_shape=(pltpu.VMEM((features, units), bf16), pltpu.VMEM((features, units), bf16),
                   pltpu.VMEM((count, width), bf16)),
        in_specs=[pl.BlockSpec(memory_space=pl.ANY if i != 1 else pltpu.VMEM) for i in range(4)],
        out_specs=[pl.BlockSpec(memory_space=pltpu.VMEM)] * 3,
        scratch_shapes=[
            pltpu.VMEM((2, rows, units), jnp.float32),
            pltpu.VMEM((count, features), bf16),
            pltpu.VMEM((count, units), bf16),
            pltpu.VMEM((n, halves, count, half_rows), bf16),
            pltpu.VMEM((n, halves, count, half_rows), bf16),
            pltpu.VMEM((groups, per_owner, halves, count, half_rows), bf16),
            dma((2, 3)), dma((2, n, chunks)),
            dma((2 * groups,)), dma((tp,)),
            dma((1,)), dma((n, halves, tiles)), dma((1,)), dma((groups, per_owner, halves, tiles)),
            dma((4,)),
        ],
        cost_estimate=pl.CostEstimate(flops=flops, bytes_accessed=4 * features * units * 2, transcendentals=0),
        compiler_params=pltpu.CompilerParams(
            collective_id=0, has_side_effects=True, vmem_limit_bytes=44 << 20),
    )(tokens, norm_gain[None, :], up_weight, down_weight)
    return tuple(pl.pallas_call(
        store,
        out_shape=[jax.ShapeDtypeStruct(r.shape, r.dtype) for r in results],
        in_specs=[pl.BlockSpec(memory_space=pl.ANY)] * 3,
        out_specs=[pl.BlockSpec(memory_space=pltpu.HBM)] * 3,
        scratch_shapes=[dma((3, pieces))],
        compiler_params=pltpu.CompilerParams(vmem_limit_bytes=1 << 20),
    )(*results))


def solution(mesh):
    return jax.shard_map(
        functools.partial(on_device, mesh.shape["fs"], mesh.shape["tp"]),
        mesh=mesh,
        in_specs=(P("fs", "tp"), P("fs"), P("fs", "tp"), P("fs", "tp")),
        out_specs=(P(None, "tp"), P(None, "tp"), P("fs", "tp")),
        check_vma=False,
    )
```

```python
import functools

import jax
import jax.numpy as jnp
from jax import lax
from jax.experimental import pallas as pl
from jax.experimental.pallas import tpu as pltpu
from jax.sharding import PartitionSpec as P

epsilon = 1e-06
MESH = pl.DeviceIdType.MESH
UP, DOWN, SIDE = 0, 1, 2


def chunks_of(rows, m):
    extra = max(16, rows * (5 + m) // 32 // 8 * 8)
    main, half = rows - extra, rows // 2
    if half % 128 == 0:
        return [(0, half), (half, main - half), (main, extra)]
    return [(0, main), (main, extra)]


def kernel(n, tp, tok_in, gain, up_weight, down_weight, up, down, total,
           stage, tok, hidden, part, pair, cross,
           send_sem, recv_sem, tok_send, tok_recv, pair_send, pair_recv, cross_send, cross_recv, local_sem, gain_row):
    rows, units = up_weight.shape
    tokens, width = tok_in.shape
    chain = n // 2
    groups = tp // 2
    per_owner = n // tp
    chunks = [chunks_of(rows, 0), chunks_of(rows, 1)]
    extra = len(chunks[0]) - 1
    mains = range(extra)
    halves = extra
    half_rows = rows // halves
    fs, me = lax.axis_index("fs"), lax.axis_index("tp")
    z, y = fs // 2, fs % 2
    group, core = me // 2, me % 2
    partner = group * 2 + 1 - core
    bufs = (up, down)

    def target(way):
        if way == UP:
            return {"fs": jnp.minimum(z + 1, chain - 1) * 2 + y}
        if way == DOWN:
            return {"fs": jnp.maximum(z - 1, 0) * 2 + y}
        return {"fs": z * 2 + 1 - y}

    def spot(m, src, k):
        return pl.ds(pl.multiple_of(pl.multiple_of(src * rows, 16) + chunks[m][k][0], 8), chunks[m][k][1])

    def copy(m, src, k, way):
        where = spot(m, src, k)
        return pltpu.make_async_remote_copy(
            src_ref=bufs[m].at[where],
            dst_ref=bufs[m].at[where],
            send_sem=send_sem.at[m, way],
            recv_sem=recv_sem.at[m, src, k],
            device_id=target(way),
            device_id_type=MESH,
        )

    def arrived(m, src, k):
        where = spot(m, src, k)
        pltpu.make_async_remote_copy(
            src_ref=bufs[m].at[where], dst_ref=bufs[m].at[where],
            send_sem=send_sem.at[m, SIDE], recv_sem=recv_sem.at[m, src, k],
            device_id=target(SIDE), device_id_type=MESH,
        ).wait_recv()

    along = [(way, k) for k in mains for way in (UP, DOWN)]
    beside = [(SIDE, extra)] + [(SIDE, k) for k in mains]

    def when_way(way, fn):
        if way == UP:
            pl.when(z < chain - 1)(fn)
        elif way == DOWN:
            pl.when(z > 0)(fn)
        else:
            fn()

    def start_own(m, order):
        for way, k in order:
            when_way(way, lambda way=way, k=k: copy(m, fs, k, way).start())

    middle = (z > 0) & (z < chain - 1)
    opposite = z * 2 + 1 - y

    def own_extras(m, late):
        for way in (UP, DOWN):
            edge = middle & (z == (chain - 2 if way == UP else 1))
            now = edge if late else jnp.logical_not(edge)

            def send(way=way):
                copy(m, fs, extra, way).start()
                copy(m, opposite, extra, way).start()

            when_way(way, lambda now=now, send=send: pl.when(now)(send))

    def step_sends(m, d, act, wait, plan):
        for k, flip in plan:
            for sign, way in ((-1, UP), (1, DOWN)):
                at = z + sign * d
                src = at * 2 + (y + flip) % 2

                @pl.when((at >= 0) & (at < chain))
                def _():
                    if wait:
                        arrived(m, src, k)
                    when_way(way, lambda: act(copy(m, src, k, way)))
                    if k != extra:
                        act(copy(m, src, k, SIDE))

    def side_arrivals(m, d):
        for sign in (-1, 1) if not (isinstance(d, int) and d == 0) else (1,):
            at = z + sign * d

            @pl.when((at >= 0) & (at < chain))
            def _():
                for k in mains:
                    arrived(m, at * 2 + 1 - y, k)

    main_plan = [(k, 0) for k in mains]
    extra_plan = [(extra, 0), (extra, 1)]

    def forward(m, d, plan):
        step_sends(m, d, lambda c: c.start(), True, plan)

    own_rows = pl.ds(pl.multiple_of(fs * rows, 16), rows)
    lead = chunks[0][0][1]
    lead_rows, other_rows = pl.ds(0, lead), pl.ds(lead, rows - lead)
    loads = [pltpu.make_async_copy(up_weight.at[lead_rows], stage.at[0, lead_rows], local_sem.at[0]),
             pltpu.make_async_copy(up_weight.at[other_rows], stage.at[0, other_rows], local_sem.at[1]),
             pltpu.make_async_copy(tok_in, tok.at[:, pl.ds(pl.multiple_of(me * width, 128), width)], local_sem.at[2]),
             pltpu.make_async_copy(down_weight, stage.at[1], local_sem.at[3])]
    gain_load = pltpu.make_async_copy(gain, gain_row, local_sem.at[4])
    gain_load.start()
    for load in loads[:2]:
        load.start()

    barrier = pltpu.get_barrier_semaphore()
    greet = [target(SIDE), {"tp": partner}]
    greet += [{"tp": lax.rem(group + g, groups) * 2 + core} for g in range(1, groups)]

    def hello(who):
        pl.semaphore_signal(barrier, inc=1, device_id=who, device_id_type=MESH)

    for way in (UP, DOWN):
        when_way(way, lambda way=way: hello(target(way)))
    for who in greet:
        hello(who)
    callers = len(greet) + (z > 0).astype(jnp.int32) + (z < chain - 1).astype(jnp.int32)
    gain_load.wait()
    by_row = jnp.transpose(jnp.broadcast_to(gain_row[...], (128, rows)))[:, :1]

    def scaled(first, count):
        at = pl.ds(pl.multiple_of(fs * rows + first, 16), count)
        up[at, :] = (by_row[first:first + count] * stage[0, first:first + count]).astype(jnp.bfloat16)

    loads[0].wait()
    for load in loads[2:]:
        load.start()
    scaled(0, lead)
    pl.semaphore_wait(barrier, callers)
    behind = (core == 1) & (z < chain // 2)
    leading = [(way, 0) for way in (UP, DOWN, SIDE)]
    following = [(way, k) for k in mains[1:] for way in (UP, DOWN, SIDE)] + [(SIDE, extra)]
    pl.when(jnp.logical_not(behind))(lambda: start_own(0, leading))
    loads[1].wait()
    scaled(lead, rows - lead)
    pl.when(jnp.logical_not(behind))(lambda: start_own(0, following))
    loads[2].wait()

    def columns(owner):
        return pl.ds(pl.multiple_of(owner * width, 128), width)

    def token_copy(owner, to, slot):
        return pltpu.make_async_remote_copy(
            src_ref=tok.at[:, columns(owner)],
            dst_ref=tok.at[:, columns(owner)],
            send_sem=tok_send.at[slot], recv_sem=tok_recv.at[owner],
            device_id={"tp": to}, device_id_type=MESH)

    across = [lax.rem(group + g, groups) * 2 + core for g in range(1, groups)]
    back = [lax.rem(group + groups - g, groups) * 2 + core for g in range(1, groups)]
    token_sends = [token_copy(me, to, i) for i, to in enumerate(across)]
    token_sends.append(token_copy(me, partner, groups - 1))
    for c in token_sends:
        c.start()
    loads[3].wait()
    down[own_rows, :] = stage[1].astype(jnp.bfloat16)
    pl.when(behind)(lambda: start_own(0, leading + following))

    forward(0, 1, main_plan)
    arrived(0, opposite, extra)
    own_extras(0, False)
    own_extras(0, True)
    pl.when(jnp.logical_not(middle))(lambda: start_own(1, along))

    relays = []
    for i, owner in enumerate(back):
        token_copy(owner, partner, groups + i).wait_recv()
        c = token_copy(owner, partner, groups + i)
        c.start()
        relays.append(c)
    forward(0, 2, main_plan)
    token_copy(partner, partner, 0).wait_recv()
    for g in range(1, groups):
        token_copy(lax.rem(group + g, groups) * 2 + 1 - core, partner, 0).wait_recv()
    for c in token_sends + relays:
        c.wait_send()
    tile = 128

    @pl.loop(0, tokens // tile)
    def _(i):
        at = pl.ds(pl.multiple_of(i * tile, tile), tile)
        wide = tok[at, :].astype(jnp.float32)
        scale = lax.rsqrt(jnp.mean(wide * wide, axis=-1, keepdims=True) + epsilon)
        tok[at, :] = (wide * scale).astype(jnp.bfloat16)

    for d in range(3, chain):
        forward(0, d, main_plan)
    start_own(1, beside)
    for d in range(1, chain):
        forward(0, d, extra_plan)
    pl.when(middle)(lambda: start_own(1, along))
    for d in range(chain):
        side_arrivals(0, d)
    bm, bn = min(512, tokens), min(512, units)

    def expand(first, last):
        @pl.loop(first, last)
        def _(j):
            cols = pl.ds(pl.multiple_of(j * bn, bn), bn)

            @pl.loop(0, tokens // bm)
            def _(i):
                at = pl.ds(pl.multiple_of(i * bm, bm), bm)
                values = jnp.dot(tok[at, :], up[:, cols], preferred_element_type=jnp.float32)
                values = jnp.maximum(values, 0.0)
                hidden[at, cols] = (values * values).astype(jnp.bfloat16)

    parts = units // bn
    expand(0, parts // 2)
    arrived(1, opposite, extra)
    own_extras(1, False)
    forward(1, 1, main_plan[:1])
    expand(parts // 2, parts * 3 // 4)
    forward(1, 1, main_plan[1:])
    expand(parts * 3 // 4, parts)

    tiles = tokens // bm

    def tile_rows(i):
        return pl.ds(pl.multiple_of(i * bm, bm), bm)

    def pair_copy(r, h, i):
        return pltpu.make_async_remote_copy(
            src_ref=part.at[r, h, tile_rows(i)], dst_ref=pair.at[r, h, tile_rows(i)],
            send_sem=pair_send.at[0], recv_sem=pair_recv.at[r // (2 * per_owner) * per_owner + r % per_owner, h, i],
            device_id={"tp": partner}, device_id_type=MESH)

    def cross_copy(r, h, i, to_group, from_group):
        slot = r % per_owner
        return pltpu.make_async_remote_copy(
            src_ref=part.at[r, h, tile_rows(i)], dst_ref=cross.at[from_group, slot, h, tile_rows(i)],
            send_sem=cross_send.at[0], recv_sem=cross_recv.at[from_group, slot, h, i],
            device_id={"tp": to_group * 2 + core}, device_id_type=MESH)

    def multiply(r, hs, after=lambda i: None):
        where = pl.ds(pl.multiple_of(r * rows + hs[0] * half_rows, 16), len(hs) * half_rows)

        @pl.loop(0, tiles)
        def _(i):
            at = tile_rows(i)
            values = lax.dot_general(
                hidden[at, :], down[where, :], (((1,), (1,)), ((), ())),
                preferred_element_type=jnp.float32).astype(jnp.bfloat16)
            for i_h, h in enumerate(hs):
                part[r, h, at, :] = values[:, i_h * half_rows:(i_h + 1) * half_rows]

            @pl.when(r // per_owner % 2 != core)
            def _():
                for h in hs:
                    pair_copy(r, h, i).start()

            after(i)

    def pair_tile(r, hs, i):
        owner = r // per_owner

        @pl.when(owner % 2 == core)
        def _():
            at = tile_rows(i)
            for h in hs:
                pair_copy(r, h, i).wait_recv()
                both = part[r, h, at, :].astype(jnp.float32) + pair[r, h, at, :].astype(jnp.float32)
                part[r, h, at, :] = both.astype(jnp.bfloat16)
                pl.when(owner // 2 != group)(lambda h=h: cross_copy(r, h, i, owner // 2, group).start())

    def pair_sum(r, hs):
        if hs:
            pl.loop(0, tiles)(lambda i: pair_tile(r, hs, i))

    def eager(r, hs):
        return lambda i: pair_tile(r, hs, i)

    def at_distance(d, flip, fn):
        for sign in (-1, 1):
            at = z + sign * d

            @pl.when((at >= 0) & (at < chain))
            def _():
                fn(at * 2 + (y + flip) % 2)

    every = list(range(halves))

    first, rest = every[:1], every[1:]
    last = chain - 1
    outer = (z <= 1) | (z >= last - 1)
    final = jnp.where(z <= 1, last, 0) * 2 + 1 - y
    head, tail = (first, rest) if rest else ([], every)

    def opposite_block(h):
        arrived(1, opposite, h)
        multiply(opposite, [h])

    def final_block():
        arrived(1, final, every[-1])
        multiply(final, every[-1:], eager(final, every[-1:]))

    def near_flow():
        def side(d, hs):
            def run(r):
                for h in hs:
                    arrived(1, r, h)
                    multiply(r, [h])

            at_distance(d, 1, run)

        def sums(d, flip, hs):
            at_distance(d, flip, lambda r: pair_sum(r, hs))

        if head:
            at_distance(1, 0, lambda r: multiply(r, head))

        @pl.loop(2, last)
        def _(d):
            forward(1, d, main_plan)

        @pl.loop(1, last - 1)
        def _(d):
            forward(1, d, extra_plan)

        forward(1, last - 1, extra_plan[:1])
        own_extras(1, True)
        forward(1, last - 1, extra_plan[1:])
        pair_sum(opposite, first)
        sums(1, 0, head)
        for h in rest:
            opposite_block(h)
        at_distance(1, 0, lambda r: multiply(r, tail))
        pair_sum(opposite, rest)

        @pl.loop(2, last)
        def _(d):
            at_distance(d, 0, lambda r: multiply(r, every))

        sums(1, 0, tail)
        side(1, first)

        @pl.loop(2, last)
        def _(d):
            sums(d, 0, every)

        sums(1, 1, first)
        side(1, rest)
        sums(1, 1, rest)

        @pl.loop(2, last - 1)
        def _(d):
            side(d, every)
            sums(d, 1, every)

        @pl.when(outer)
        def _():
            before = every[:-1]
            for h in before:
                arrived(1, final, h)
                multiply(final, [h], eager(final, [h]))
            final_block()

    def end_flow():
        def far(d, flip):
            return jnp.where(z == 0, d, last - d) * 2 + (y + flip) % 2

        def take(d, k, flip=0):
            r = far(d, flip)
            arrived(1, r, k)
            if k != extra:
                copy(1, r, k, SIDE).start()

        def main(d, hs, soon=False):
            r = far(d, 0)
            if hs:
                multiply(r, hs, *([eager(r, hs)] if soon else []))

        def side(d, hs, soon=False):
            r = far(d, 1)
            for h in hs:
                arrived(1, r, h)
                multiply(r, [h], *([eager(r, [h])] if soon else []))

        def sums(d, flip, hs):
            pair_sum(far(d, flip), hs)

        main(1, head)
        pair_sum(opposite, first)
        for h in rest:
            opposite_block(h)
        sums(1, 0, head)
        pair_sum(opposite, rest)

        @pl.loop(2, chain)
        def _(d):
            take(d, 0)
            main(d, head)
            sums(d, 0, head)
            side(d - 1, head)
            for k in mains[1:]:
                take(d, k)
            sums(d - 1, 1, head)

        @pl.loop(2, last)
        def _(d):
            take(d, extra)
            main(d, tail)
            take(d, extra, 1)
            sums(d, 0, tail)
            side(d, tail)
            sums(d, 1, tail)

        take(last, extra)
        main(last, tail, True)
        take(1, extra)
        main(1, tail, True)
        side(last, head, True)
        take(1, extra, 1)
        side(1, tail, True)
        take(last, extra, 1)
        final_block()

    multiply(fs, every)
    opposite_block(0)
    pair_sum(fs, every)
    pl.when(middle)(near_flow)
    pl.when(jnp.logical_not(middle))(end_flow)

    for s in range(per_owner):
        r = me * per_owner + s
        for h in every:
            first_column = s * rows + h * half_rows

            @pl.loop(0, tiles)
            def _(i):
                at = tile_rows(i)
                value = part[r, h, at, :].astype(jnp.float32)
                for g in range(1, groups):
                    other = lax.rem(group + g, groups)
                    cross_copy(r, h, i, other, other).wait_recv()
                    value = value + cross[other, s, h, at, :].astype(jnp.float32)
                total[at, first_column:first_column + half_rows] = value.astype(jnp.bfloat16)

    for m in (0, 1):
        spread = rows + chunks[m][extra][1]

        def sent(way, count):
            where = pl.ds(0, count)
            pltpu.make_async_remote_copy(
                src_ref=bufs[m].at[where], dst_ref=bufs[m].at[where],
                send_sem=send_sem.at[m, way], recv_sem=recv_sem.at[m, fs, 0],
                device_id=target(way), device_id_type=MESH).wait_send()

        sent(SIDE, rows + (chain - 1) * (rows - chunks[m][extra][1]))
        for i in range(last):
            pl.when(z == i)(lambda i=i: sent(UP, (i + 1) * spread))
            pl.when(z == last - i)(lambda i=i: sent(DOWN, (i + 1) * spread))

    def all_sent(sem, recv, count, who):
        where = pl.ds(0, count)
        pltpu.make_async_remote_copy(
            src_ref=part.at[where], dst_ref=part.at[where], send_sem=sem, recv_sem=recv,
            device_id={"tp": who}, device_id_type=MESH).wait_send()

    all_sent(pair_send.at[0], pair_recv.at[0, 0, 0], n // 2, partner)
    if groups > 1:
        all_sent(cross_send.at[0], cross_recv.at[0, 0, 0, 0], per_owner * (groups - 1), partner)


pieces = 2


def store(up, down, total, up_out, down_out, total_out, sem):
    copies = []
    for i, (src, dst) in enumerate(((up, up_out), (down, down_out), (total, total_out))):
        step = src.shape[0] // pieces
        for j in range(pieces):
            at = pl.ds(j * step, step)
            copies.append(pltpu.make_async_copy(src.at[at], dst.at[at], sem.at[i, j]))
    for c in copies:
        c.start()
    for c in copies:
        c.wait()


def on_device(n, tp, tokens, norm_gain, up_weight, down_weight):
    rows, units = up_weight.shape
    count, width = tokens.shape
    bf16 = jnp.bfloat16
    groups, per_owner = tp // 2, n // tp
    chunks = len(chunks_of(rows, 0))
    halves = chunks - 1
    half_rows = rows // halves
    features = width * tp
    tiles = count // min(512, count)
    dma = pltpu.SemaphoreType.DMA
    flops = 2 * 2 * count * features * units
    results = pl.pallas_call(
        functools.partial(kernel, n, tp),
        out_shape=(pltpu.VMEM((features, units), bf16), pltpu.VMEM((features, units), bf16),
                   pltpu.VMEM((count, width), bf16)),
        in_specs=[pl.BlockSpec(memory_space=pl.ANY)] * 4,
        out_specs=[pl.BlockSpec(memory_space=pltpu.VMEM)] * 3,
        scratch_shapes=[
            pltpu.VMEM((2, rows, units), jnp.float32),
            pltpu.VMEM((count, features), bf16),
            pltpu.VMEM((count, units), bf16),
            pltpu.VMEM((n, halves, count, half_rows), bf16),
            pltpu.VMEM((n, halves, count, half_rows), bf16),
            pltpu.VMEM((groups, per_owner, halves, count, half_rows), bf16),
            dma((2, 3)), dma((2, n, chunks)),
            dma((2 * groups,)), dma((tp,)),
            dma((1,)), dma((n // 2, halves, tiles)), dma((1,)), dma((groups, per_owner, halves, tiles)),
            dma((5,)), pltpu.VMEM((1, rows), jnp.float32),
        ],
        cost_estimate=pl.CostEstimate(flops=flops, bytes_accessed=4 * features * units * 2, transcendentals=0),
        compiler_params=pltpu.CompilerParams(
            collective_id=0, has_side_effects=True, vmem_limit_bytes=44 << 20),
    )(tokens, norm_gain[None, :], up_weight, down_weight)
    return tuple(pl.pallas_call(
        store,
        out_shape=[jax.ShapeDtypeStruct(r.shape, r.dtype) for r in results],
        in_specs=[pl.BlockSpec(memory_space=pl.ANY)] * 3,
        out_specs=[pl.BlockSpec(memory_space=pltpu.HBM)] * 3,
        scratch_shapes=[dma((3, pieces))],
        compiler_params=pltpu.CompilerParams(vmem_limit_bytes=1 << 20),
    )(*results))


def solution(mesh):
    return jax.shard_map(
        functools.partial(on_device, mesh.shape["fs"], mesh.shape["tp"]),
        mesh=mesh,
        in_specs=(P("fs", "tp"), P("fs"), P("fs", "tp"), P("fs", "tp")),
        out_specs=(P(None, "tp"), P(None, "tp"), P("fs", "tp")),
        check_vma=False,
    )
```

```python
import functools

import jax
import jax.numpy as jnp
from jax import lax
from jax.experimental import pallas as pl
from jax.experimental.pallas import tpu as pltpu
from jax.sharding import PartitionSpec as P

epsilon = 1e-06
MESH = pl.DeviceIdType.MESH
UP, DOWN, SIDE = 0, 1, 2


def chunks_of(rows, m):
    extra = max(16, rows * (5 + m) // 32 // 8 * 8)
    main, half = rows - extra, rows // 2
    if half % 128 == 0:
        return [(0, half), (half, main - half), (main, extra)]
    return [(0, main), (main, extra)]


def kernel(n, tp, tok_in, gain, up_weight, down_weight, up, down, total,
           stage, tok, hidden, part, pair, cross,
           send_sem, recv_sem, tok_send, tok_recv, pair_send, pair_recv, cross_send, cross_recv, local_sem, gain_row):
    rows, units = up_weight.shape
    tokens, width = tok_in.shape
    chain = n // 2
    groups = tp // 2
    per_owner = n // tp
    chunks = [chunks_of(rows, 0), chunks_of(rows, 1)]
    extra = len(chunks[0]) - 1
    mains = range(extra)
    halves = extra
    half_rows = rows // halves
    fs, me = lax.axis_index("fs"), lax.axis_index("tp")
    z, y = fs // 2, fs % 2
    group, core = me // 2, me % 2
    partner = group * 2 + 1 - core
    bufs = (up, down)

    def target(way):
        if way == UP:
            return {"fs": jnp.minimum(z + 1, chain - 1) * 2 + y}
        if way == DOWN:
            return {"fs": jnp.maximum(z - 1, 0) * 2 + y}
        return {"fs": z * 2 + 1 - y}

    def spot(m, src, k):
        return pl.ds(pl.multiple_of(pl.multiple_of(src * rows, 16) + chunks[m][k][0], 8), chunks[m][k][1])

    def copy(m, src, k, way):
        where = spot(m, src, k)
        return pltpu.make_async_remote_copy(
            src_ref=bufs[m].at[where],
            dst_ref=bufs[m].at[where],
            send_sem=send_sem.at[m, way],
            recv_sem=recv_sem.at[m, src, k],
            device_id=target(way),
            device_id_type=MESH,
        )

    def arrived(m, src, k):
        where = spot(m, src, k)
        pltpu.make_async_remote_copy(
            src_ref=bufs[m].at[where], dst_ref=bufs[m].at[where],
            send_sem=send_sem.at[m, SIDE], recv_sem=recv_sem.at[m, src, k],
            device_id=target(SIDE), device_id_type=MESH,
        ).wait_recv()

    along = [(way, k) for k in mains for way in (UP, DOWN)]
    beside = [(SIDE, extra)] + [(SIDE, k) for k in mains]

    def when_way(way, fn):
        if way == UP:
            pl.when(z < chain - 1)(fn)
        elif way == DOWN:
            pl.when(z > 0)(fn)
        else:
            fn()

    def start_own(m, order):
        for way, k in order:
            when_way(way, lambda way=way, k=k: copy(m, fs, k, way).start())

    middle = (z > 0) & (z < chain - 1)
    opposite = z * 2 + 1 - y

    def own_extras(m, late):
        for way in (UP, DOWN):
            edge = middle & (z == (chain - 2 if way == UP else 1))
            now = edge if late else jnp.logical_not(edge)

            def send(way=way):
                copy(m, fs, extra, way).start()
                copy(m, opposite, extra, way).start()

            when_way(way, lambda now=now, send=send: pl.when(now)(send))

    def step_sends(m, d, act, wait, plan):
        for k, flip in plan:
            for sign, way in ((-1, UP), (1, DOWN)):
                at = z + sign * d
                src = at * 2 + (y + flip) % 2

                @pl.when((at >= 0) & (at < chain))
                def _():
                    if wait:
                        arrived(m, src, k)
                    when_way(way, lambda: act(copy(m, src, k, way)))
                    if k != extra:
                        act(copy(m, src, k, SIDE))

    def side_arrivals(m, d):
        for sign in (-1, 1) if not (isinstance(d, int) and d == 0) else (1,):
            at = z + sign * d

            @pl.when((at >= 0) & (at < chain))
            def _():
                for k in mains:
                    arrived(m, at * 2 + 1 - y, k)

    main_plan = [(k, 0) for k in mains]
    extra_plan = [(extra, 0), (extra, 1)]

    def forward(m, d, plan):
        step_sends(m, d, lambda c: c.start(), True, plan)

    own_rows = pl.ds(pl.multiple_of(fs * rows, 16), rows)
    lead = chunks[0][0][1]
    lead_rows, other_rows = pl.ds(0, lead), pl.ds(lead, rows - lead)
    loads = [pltpu.make_async_copy(up_weight.at[lead_rows], stage.at[0, lead_rows], local_sem.at[0]),
             pltpu.make_async_copy(up_weight.at[other_rows], stage.at[0, other_rows], local_sem.at[1]),
             pltpu.make_async_copy(tok_in, tok.at[:, pl.ds(pl.multiple_of(me * width, 128), width)], local_sem.at[2]),
             pltpu.make_async_copy(down_weight, stage.at[1], local_sem.at[3])]
    gain_load = pltpu.make_async_copy(gain, gain_row, local_sem.at[4])
    gain_load.start()
    for load in loads[:2]:
        load.start()

    barrier = pltpu.get_barrier_semaphore()
    greet = [target(SIDE), {"tp": partner}]
    greet += [{"tp": lax.rem(group + g, groups) * 2 + core} for g in range(1, groups)]

    def hello(who):
        pl.semaphore_signal(barrier, inc=1, device_id=who, device_id_type=MESH)

    for way in (UP, DOWN):
        when_way(way, lambda way=way: hello(target(way)))
    for who in greet:
        hello(who)
    callers = len(greet) + (z > 0).astype(jnp.int32) + (z < chain - 1).astype(jnp.int32)
    gain_load.wait()
    by_row = jnp.transpose(jnp.broadcast_to(gain_row[...], (128, rows)))[:, :1]

    def scaled(first, count):
        at = pl.ds(pl.multiple_of(fs * rows + first, 16), count)
        up[at, :] = (by_row[first:first + count] * stage[0, first:first + count]).astype(jnp.bfloat16)

    loads[0].wait()
    for load in loads[2:]:
        load.start()
    scaled(0, lead)
    pl.semaphore_wait(barrier, callers)
    behind = (core == 1) & (z < chain // 2)
    leading = [(way, 0) for way in (UP, DOWN, SIDE)]
    following = [(way, k) for k in mains[1:] for way in (UP, DOWN, SIDE)] + [(SIDE, extra)]
    pl.when(jnp.logical_not(behind))(lambda: start_own(0, leading))
    loads[1].wait()
    scaled(lead, rows - lead)
    pl.when(jnp.logical_not(behind))(lambda: start_own(0, following))
    loads[2].wait()

    def columns(owner):
        return pl.ds(pl.multiple_of(owner * width, 128), width)

    def token_copy(owner, to, slot):
        return pltpu.make_async_remote_copy(
            src_ref=tok.at[:, columns(owner)],
            dst_ref=tok.at[:, columns(owner)],
            send_sem=tok_send.at[slot], recv_sem=tok_recv.at[owner],
            device_id={"tp": to}, device_id_type=MESH)

    across = [lax.rem(group + g, groups) * 2 + core for g in range(1, groups)]
    back = [lax.rem(group + groups - g, groups) * 2 + core for g in range(1, groups)]
    token_sends = [token_copy(me, to, i) for i, to in enumerate(across)]
    token_sends.append(token_copy(me, partner, groups - 1))
    for c in token_sends:
        c.start()
    loads[3].wait()
    down[own_rows, :] = stage[1].astype(jnp.bfloat16)
    pl.when(behind)(lambda: start_own(0, leading + following))

    forward(0, 1, main_plan)
    arrived(0, opposite, extra)
    own_extras(0, False)
    own_extras(0, True)
    pl.when(jnp.logical_not(middle))(lambda: start_own(1, along))

    relays = []
    for i, owner in enumerate(back):
        token_copy(owner, partner, groups + i).wait_recv()
        c = token_copy(owner, partner, groups + i)
        c.start()
        relays.append(c)
    forward(0, 2, main_plan)
    token_copy(partner, partner, 0).wait_recv()
    for g in range(1, groups):
        token_copy(lax.rem(group + g, groups) * 2 + 1 - core, partner, 0).wait_recv()
    for c in token_sends + relays:
        c.wait_send()
    tile = 128

    @pl.loop(0, tokens // tile)
    def _(i):
        at = pl.ds(pl.multiple_of(i * tile, tile), tile)
        wide = tok[at, :].astype(jnp.float32)
        scale = lax.rsqrt(jnp.mean(wide * wide, axis=-1, keepdims=True) + epsilon)
        tok[at, :] = (wide * scale).astype(jnp.bfloat16)

    for d in range(3, chain):
        forward(0, d, main_plan)
    start_own(1, beside)
    for d in range(1, chain):
        forward(0, d, extra_plan)
    pl.when(middle)(lambda: start_own(1, along))
    for d in range(chain):
        side_arrivals(0, d)
    bm, bn = min(512, tokens), min(512, units)

    def expand(first, last):
        @pl.loop(first, last)
        def _(j):
            cols = pl.ds(pl.multiple_of(j * bn, bn), bn)

            @pl.loop(0, tokens // bm)
            def _(i):
                at = pl.ds(pl.multiple_of(i * bm, bm), bm)
                values = jnp.dot(tok[at, :], up[:, cols], preferred_element_type=jnp.float32)
                values = jnp.maximum(values, 0.0)
                hidden[at, cols] = (values * values).astype(jnp.bfloat16)

    parts = units // bn
    expand(0, parts // 2)
    arrived(1, opposite, extra)
    own_extras(1, False)
    forward(1, 1, main_plan[:1])
    expand(parts // 2, parts * 3 // 4)
    forward(1, 1, main_plan[1:])
    expand(parts * 3 // 4, parts)

    tiles = tokens // bm

    def tile_rows(i):
        return pl.ds(pl.multiple_of(i * bm, bm), bm)

    def pair_copy(r, h, i):
        return pltpu.make_async_remote_copy(
            src_ref=part.at[r, h, tile_rows(i)], dst_ref=pair.at[r, h, tile_rows(i)],
            send_sem=pair_send.at[0], recv_sem=pair_recv.at[r // (2 * per_owner) * per_owner + r % per_owner, h, i],
            device_id={"tp": partner}, device_id_type=MESH)

    def cross_copy(r, h, i, to_group, from_group, into):
        slot = r % per_owner
        lane = lax.rem(from_group + groups - into + groups - 1, groups)
        return pltpu.make_async_remote_copy(
            src_ref=part.at[r, h, tile_rows(i)], dst_ref=cross.at[from_group, slot, h, tile_rows(i)],
            send_sem=cross_send.at[0], recv_sem=cross_recv.at[lane, slot, h, i],
            device_id={"tp": to_group * 2 + core}, device_id_type=MESH)

    def multiply(r, hs, after=lambda i: None):
        where = pl.ds(pl.multiple_of(r * rows + hs[0] * half_rows, 16), len(hs) * half_rows)

        @pl.loop(0, tiles)
        def _(i):
            at = tile_rows(i)
            values = lax.dot_general(
                hidden[at, :], down[where, :], (((1,), (1,)), ((), ())),
                preferred_element_type=jnp.float32).astype(jnp.bfloat16)
            for i_h, h in enumerate(hs):
                part[r, h, at, :] = values[:, i_h * half_rows:(i_h + 1) * half_rows]

            @pl.when(r // per_owner % 2 != core)
            def _():
                for h in hs:
                    pair_copy(r, h, i).start()

            after(i)

    def pair_tile(r, hs, i):
        owner = r // per_owner

        @pl.when(owner % 2 == core)
        def _():
            at = tile_rows(i)
            for h in hs:
                pair_copy(r, h, i).wait_recv()
                both = part[r, h, at, :].astype(jnp.float32) + pair[r, h, at, :].astype(jnp.float32)
                part[r, h, at, :] = both.astype(jnp.bfloat16)
                pl.when(owner // 2 != group)(lambda h=h: cross_copy(r, h, i, owner // 2, group, owner // 2).start())

    def pair_sum(r, hs):
        if hs:
            pl.loop(0, tiles)(lambda i: pair_tile(r, hs, i))

    def eager(r, hs):
        return lambda i: pair_tile(r, hs, i)

    def at_distance(d, flip, fn):
        for sign in (-1, 1):
            at = z + sign * d

            @pl.when((at >= 0) & (at < chain))
            def _():
                fn(at * 2 + (y + flip) % 2)

    every = list(range(halves))

    first, rest = every[:1], every[1:]
    last = chain - 1
    outer = (z <= 1) | (z >= last - 1)
    final = jnp.where(z <= 1, last, 0) * 2 + 1 - y
    head, tail = (first, rest) if rest else ([], every)

    def opposite_block(h):
        arrived(1, opposite, h)
        multiply(opposite, [h])

    def final_block():
        arrived(1, final, every[-1])
        multiply(final, every[-1:], eager(final, every[-1:]))

    def near_flow():
        def side(d, hs):
            def run(r):
                for h in hs:
                    arrived(1, r, h)
                    multiply(r, [h])

            at_distance(d, 1, run)

        def sums(d, flip, hs):
            at_distance(d, flip, lambda r: pair_sum(r, hs))

        if head:
            at_distance(1, 0, lambda r: multiply(r, head))

        @pl.loop(2, last)
        def _(d):
            forward(1, d, main_plan)

        @pl.loop(1, last - 1)
        def _(d):
            forward(1, d, extra_plan)

        forward(1, last - 1, extra_plan[:1])
        own_extras(1, True)
        forward(1, last - 1, extra_plan[1:])
        pair_sum(opposite, first)
        sums(1, 0, head)
        for h in rest:
            opposite_block(h)
        at_distance(1, 0, lambda r: multiply(r, tail))
        pair_sum(opposite, rest)

        @pl.loop(2, last)
        def _(d):
            at_distance(d, 0, lambda r: multiply(r, every))

        sums(1, 0, tail)
        side(1, first)

        @pl.loop(2, last)
        def _(d):
            sums(d, 0, every)

        sums(1, 1, first)
        side(1, rest)
        sums(1, 1, rest)

        @pl.loop(2, last - 1)
        def _(d):
            side(d, every)
            sums(d, 1, every)

        @pl.when(outer)
        def _():
            before = every[:-1]
            for h in before:
                arrived(1, final, h)
                multiply(final, [h], eager(final, [h]))
            final_block()

    def end_flow():
        def far(d, flip):
            return jnp.where(z == 0, d, last - d) * 2 + (y + flip) % 2

        def take(d, k, flip=0):
            r = far(d, flip)
            arrived(1, r, k)
            if k != extra:
                copy(1, r, k, SIDE).start()

        def main(d, hs, soon=False):
            r = far(d, 0)
            if hs:
                multiply(r, hs, *([eager(r, hs)] if soon else []))

        def side(d, hs, soon=False):
            r = far(d, 1)
            for h in hs:
                arrived(1, r, h)
                multiply(r, [h], *([eager(r, [h])] if soon else []))

        def sums(d, flip, hs):
            pair_sum(far(d, flip), hs)

        main(1, head)
        pair_sum(opposite, first)
        for h in rest:
            opposite_block(h)
        sums(1, 0, head)
        pair_sum(opposite, rest)

        @pl.loop(2, chain)
        def _(d):
            take(d, 0)
            main(d, head)
            sums(d, 0, head)
            side(d - 1, head)
            for k in mains[1:]:
                take(d, k)
            sums(d - 1, 1, head)

        @pl.loop(2, last)
        def _(d):
            take(d, extra)
            main(d, tail)
            take(d, extra, 1)
            sums(d, 0, tail)
            side(d, tail)
            sums(d, 1, tail)

        take(last, extra)
        main(last, tail, True)
        take(1, extra)
        main(1, tail, True)
        side(last, head, True)
        take(1, extra, 1)
        side(1, tail, True)
        take(last, extra, 1)
        final_block()

    multiply(fs, every)
    opposite_block(0)
    pair_sum(fs, every)
    pl.when(middle)(near_flow)
    pl.when(jnp.logical_not(middle))(end_flow)

    for s in range(per_owner):
        r = me * per_owner + s
        for h in every:
            first_column = s * rows + h * half_rows

            @pl.loop(0, tiles)
            def _(i):
                at = tile_rows(i)
                value = part[r, h, at, :].astype(jnp.float32)
                for g in range(1, groups):
                    other = lax.rem(group + g, groups)
                    cross_copy(r, h, i, other, other, group).wait_recv()
                    value = value + cross[other, s, h, at, :].astype(jnp.float32)
                total[at, first_column:first_column + half_rows] = value.astype(jnp.bfloat16)

    for m in (0, 1):
        spread = rows + chunks[m][extra][1]

        def sent(way, count):
            where = pl.ds(0, count)
            pltpu.make_async_remote_copy(
                src_ref=bufs[m].at[where], dst_ref=bufs[m].at[where],
                send_sem=send_sem.at[m, way], recv_sem=recv_sem.at[m, fs, 0],
                device_id=target(way), device_id_type=MESH).wait_send()

        sent(SIDE, rows + (chain - 1) * (rows - chunks[m][extra][1]))
        for i in range(last):
            pl.when(z == i)(lambda i=i: sent(UP, (i + 1) * spread))
            pl.when(z == last - i)(lambda i=i: sent(DOWN, (i + 1) * spread))

    def all_sent(sem, recv, count, who):
        where = pl.ds(0, count)
        pltpu.make_async_remote_copy(
            src_ref=part.at[where], dst_ref=part.at[where], send_sem=sem, recv_sem=recv,
            device_id={"tp": who}, device_id_type=MESH).wait_send()

    all_sent(pair_send.at[0], pair_recv.at[0, 0, 0], n // 2, partner)
    if groups > 1:
        all_sent(cross_send.at[0], cross_recv.at[0, 0, 0, 0], per_owner * (groups - 1), partner)


pieces = 2


def store(up, down, total, up_out, down_out, total_out, sem):
    copies = []
    for i, (src, dst) in enumerate(((up, up_out), (down, down_out), (total, total_out))):
        step = src.shape[0] // pieces
        for j in range(pieces):
            at = pl.ds(j * step, step)
            copies.append(pltpu.make_async_copy(src.at[at], dst.at[at], sem.at[i, j]))
    for c in copies:
        c.start()
    for c in copies:
        c.wait()


def on_device(n, tp, tokens, norm_gain, up_weight, down_weight):
    rows, units = up_weight.shape
    count, width = tokens.shape
    bf16 = jnp.bfloat16
    groups, per_owner = tp // 2, n // tp
    chunks = len(chunks_of(rows, 0))
    halves = chunks - 1
    half_rows = rows // halves
    features = width * tp
    tiles = count // min(512, count)
    dma = pltpu.SemaphoreType.DMA
    flops = 2 * 2 * count * features * units
    results = pl.pallas_call(
        functools.partial(kernel, n, tp),
        out_shape=(pltpu.VMEM((features, units), bf16), pltpu.VMEM((features, units), bf16),
                   pltpu.VMEM((count, width), bf16)),
        in_specs=[pl.BlockSpec(memory_space=pl.ANY)] * 4,
        out_specs=[pl.BlockSpec(memory_space=pltpu.VMEM)] * 3,
        scratch_shapes=[
            pltpu.VMEM((2, rows, units), jnp.float32),
            pltpu.VMEM((count, features), bf16),
            pltpu.VMEM((count, units), bf16),
            pltpu.VMEM((n, halves, count, half_rows), bf16),
            pltpu.VMEM((n, halves, count, half_rows), bf16),
            pltpu.VMEM((groups, per_owner, halves, count, half_rows), bf16),
            dma((2, 3)), dma((2, n, chunks)),
            dma((2 * groups,)), dma((tp,)),
            dma((1,)), dma((n // 2, halves, tiles)), dma((1,)), dma((max(groups - 1, 1), per_owner, halves, tiles)),
            dma((5,)), pltpu.VMEM((1, rows), jnp.float32),
        ],
        cost_estimate=pl.CostEstimate(flops=flops, bytes_accessed=4 * features * units * 2, transcendentals=0),
        compiler_params=pltpu.CompilerParams(
            collective_id=0, has_side_effects=True, vmem_limit_bytes=44 << 20),
    )(tokens, norm_gain[None, :], up_weight, down_weight)
    return tuple(pl.pallas_call(
        store,
        out_shape=[jax.ShapeDtypeStruct(r.shape, r.dtype) for r in results],
        in_specs=[pl.BlockSpec(memory_space=pl.ANY)] * 3,
        out_specs=[pl.BlockSpec(memory_space=pltpu.HBM)] * 3,
        scratch_shapes=[dma((3, pieces))],
        compiler_params=pltpu.CompilerParams(vmem_limit_bytes=1 << 20),
    )(*results))


def solution(mesh):
    return jax.shard_map(
        functools.partial(on_device, mesh.shape["fs"], mesh.shape["tp"]),
        mesh=mesh,
        in_specs=(P("fs", "tp"), P("fs"), P("fs", "tp"), P("fs", "tp")),
        out_specs=(P(None, "tp"), P(None, "tp"), P("fs", "tp")),
        check_vma=False,
    )
```
